32 devices in a mesh: grp: 2 (over y), sp: 4 (over z), tp: 4 (over x, core).
Axes of the slice: x: 2, y: 2, z: 4, core: 2. Of those that a mesh axis runs over, the one named last changes fastest.
Arguments:
- residual: bfloat16 [3072, 2048], P(('grp', 'sp', 'tp')), parts along dimension 0, may hold values from -36 to 36
- query: bfloat16 [3072, 512], P(('grp', 'sp'), 'tp'), parts along dimension 0, may hold values from -6 to 6
- keys: bfloat16 [3072, 512], P(('grp', 'sp'), 'tp'), parts along dimension 0, may hold values from -6 to 6
- values: bfloat16 [3072, 1024], P(('grp', 'sp'), 'tp'), parts along dimension 0, may hold values from -6 to 6
- out_gate: bfloat16 [3072, 1024], P(('grp', 'sp'), 'tp'), parts along dimension 0, may hold values from -6 to 6
- input_gate: float32 [2, 4, 3072], P(None, 'tp', ('grp', 'sp')), parts along dimension 2, may hold values from -5 to 95
- forget_gate: float32 [2, 4, 3072], P(None, 'tp', ('grp', 'sp')), parts along dimension 2, may hold values from -6 to 20
- head_gain: float32 [1024], P('tp'), may hold values from 0.1 to 1.9
- w_out: bfloat16 [1024, 2048], P('tp'), may hold values from -0.1875 to 0.1875
- norm_gain: float32 [2048], replicated, may hold values from 0.1 to 1.9
- w_up_gate: bfloat16 [2048, 5632], P('sp', 'tp'), may hold values from -0.125 to 0.125
- w_up_value: bfloat16 [2048, 5632], P('sp', 'tp'), may hold values from -0.125 to 0.125
- conv_gate: float32 [3, 5632], P(None, 'tp'), may hold values from -3 to 3
- conv_value: float32 [3, 5632], P(None, 'tp'), may hold values from -3 to 3
- w_down: bfloat16 [5632, 2048], P('tp', 'sp'), may hold values from -0.078125 to 0.078125
Outputs:
- layer_out: bfloat16 [3072, 2048], P(('grp', 'sp', 'tp')), parts along dimension 0
The draws below stay inside these ranges and needn't reach their ends.
There are 2 independent parts, one for each index of `grp`. The reference program is written for one: setup_inputs(seed, part) draws one part's arguments, and reference() takes and returns one part's arrays. A program takes and returns all parts, laid end to end along the dimension named above; an argument that names none is the same for every part. Nothing has to cross between parts.
All inputs are finite; a program needn't handle non-finite values.
Results may differ from the reference program's by a relative error of at most 0.011.
Values may be sent and summed in bfloat16 or wider, within the bound.
A program may use at most 128 MiB of HBM per device.

```python
import math
import jax
import jax.numpy as jnp
from jax import lax

D = 2048
HEADS = 4
QK_DIM = 128
V_DIM = 256
FF = 5632
CONV = 3
TOK_DEV = 384
TOKENS = 1536
QK_WIDTH = 512
V_WIDTH = 1024


def spike_flags(key, item_count):
    spots = jax.random.randint(key, (2, HEADS, item_count), 0, TOKENS)
    places = jnp.arange(TOKENS)
    return jnp.any(places[None, None, :, None] == spots[:, :, None, :], axis=-1)


def draw_input_gate(key, part):
    sequence_lanes = jax.random.split(jax.random.fold_in(key, 11), 1)
    reference_level = jnp.clip(jax.random.normal(sequence_lanes[0], (2, HEADS, TOKENS), jnp.float32), -5.0, 5.0)
    return reference_level


def draw_forget_gate(key, part):
    sequence_lanes = jax.random.split(jax.random.fold_in(key, 23), 6)
    ranking = jnp.stack([jax.random.permutation(sequence_lanes[0], HEADS), jax.random.permutation(sequence_lanes[1], HEADS)])
    quick_heads = ranking < HEADS // 2
    head_rates = jnp.where(quick_heads, 8.0 / TOK_DEV, 0.5 / TOKENS).astype(jnp.float32)
    factor = jnp.exp(jax.random.uniform(sequence_lanes[2], (2, HEADS, TOKENS // TOK_DEV), jnp.float32, -math.log(2.0), math.log(2.0)))
    factor = jnp.repeat(factor, TOK_DEV, axis=2)
    jitter = jnp.clip(jax.random.normal(sequence_lanes[3], (2, HEADS, TOKENS), jnp.float32), -4.0, 4.0)
    stable_value = -jnp.log(head_rates[:, :, None] * factor) - 0.5 + jitter
    retained_state = jax.random.uniform(sequence_lanes[5], (2, HEADS, TOKENS), jnp.float32, 0.5, 0.8)
    return jnp.where(spike_flags(sequence_lanes[4], 3), jnp.log(retained_state / (1.0 - retained_state)), stable_value)


def draw_residual(key, part):
    sequence_lanes = jax.random.split(jax.random.fold_in(key, 37), 3)
    row_scale = jnp.exp(jax.random.uniform(sequence_lanes[0], (TOKENS, 1), jnp.float32, math.log(0.3), math.log(3.0)))
    column_scale = jnp.exp(jax.random.uniform(sequence_lanes[1], (1, D), jnp.float32, math.log(0.3), math.log(3.0)))
    entries = jnp.clip(jax.random.normal(sequence_lanes[2], (TOKENS, D), jnp.float32), -4.0, 4.0)
    return (entries * row_scale * column_scale).astype(jnp.bfloat16)


def levels(key, extent, cuts, low, high):
    level, own = 1.0, jax.random.fold_in(key, 6)
    for position, parts in cuts:
        draws = jnp.exp(jax.random.uniform(jax.random.fold_in(own, position), (parts,), jnp.float32, low / len(cuts), high / len(cuts)))
        level = level * jnp.repeat(draws, extent[position] // parts).reshape([-1 if axis == position else 1 for axis in range(len(extent))])
    return level


def normal_values(stream_key, extent, spread, limit, cuts=(), held_as=jnp.bfloat16):
    level = levels(stream_key, extent, cuts, -0.22, 0.18) if cuts else 1.0
    drawn = jax.random.normal(stream_key, extent, jnp.float32) * spread * level
    return jnp.minimum(jnp.maximum(drawn, -limit), limit).astype(held_as)


def setup_inputs(seed: int = 0, part: int = 0) -> dict:
    key_list = jax.random.split(jax.random.key(seed), 16)
    part_keys = jax.random.split(jax.random.fold_in(key_list[15], part), 16)
    residual = draw_residual(jax.random.fold_in(jax.random.fold_in(key_list[15], part), 71), part)
    query = normal_values(part_keys[1], (TOKENS, QK_WIDTH), 1.0, 6.0, ((0, 4), (1, 4)))
    keys = normal_values(part_keys[2], (TOKENS, QK_WIDTH), 1.0, 6.0, ((0, 4), (1, 4)))
    values = normal_values(part_keys[3], (TOKENS, V_WIDTH), 1.0, 6.0, ((0, 4), (1, 4)))
    out_gate = normal_values(part_keys[4], (TOKENS, V_WIDTH), 1.5, 6.0, ((0, 4), (1, 4)))
    input_gate = draw_input_gate(jax.random.fold_in(jax.random.fold_in(key_list[15], part), 71), part)
    forget_gate = draw_forget_gate(jax.random.fold_in(jax.random.fold_in(key_list[15], part), 71), part)
    head_gain = jnp.clip(1.0 + 0.18 * jax.random.normal(key_list[7], (V_WIDTH,), jnp.float32), 0.1, 1.9)
    w_out = normal_values(key_list[8], (V_WIDTH, D), V_WIDTH ** -0.5, 0.1875, ((0, 4),))
    norm_gain = jnp.clip(1.0 + 0.18 * jax.random.normal(key_list[9], (D,), jnp.float32), 0.1, 1.9)
    w_up_gate = normal_values(key_list[10], (D, FF), D ** -0.5, 0.125, ((0, 4), (1, 4)))
    w_up_value = normal_values(key_list[11], (D, FF), D ** -0.5, 0.125, ((0, 4), (1, 4)))
    conv_gate = normal_values(key_list[12], (CONV, FF), 0.577, 3.0, ((1, 4),), jnp.float32)
    conv_value = normal_values(key_list[13], (CONV, FF), 0.577, 3.0, ((1, 4),), jnp.float32)
    w_down = normal_values(key_list[14], (FF, D), FF ** -0.5, 0.078125, ((0, 4), (1, 4)))
    return {"residual": residual, "query": query, "keys": keys, "values": values, "out_gate": out_gate, "input_gate": input_gate, "forget_gate": forget_gate, "head_gain": head_gain, "w_out": w_out, "norm_gain": norm_gain, "w_up_gate": w_up_gate, "w_up_value": w_up_value, "conv_gate": conv_gate, "conv_value": conv_value, "w_down": w_down}


epsilon = 1e-06
floor_log = -1e+30
highest = lax.Precision.HIGHEST

def summarize(keys_scaled, values_wide, in_gate, log_cum):
    totals = log_cum[:, -1]
    growth = totals[:, None] - log_cum + in_gate
    largest = lax.optimization_barrier(jnp.max(growth, axis=-1))
    weighting = jnp.exp(growth - largest[:, None])
    weighted = keys_scaled * jnp.transpose(weighting)[:, :, None]
    memory = jnp.einsum('shd,she->hde', weighted, values_wide, precision=highest)
    return (totals, memory, lax.optimization_barrier(jnp.sum(weighted, axis=0)), largest)

def combine(early, later):
    early_total, early_memory, early_normalizer, early_top = early
    later_total, later_memory, later_normalizer, later_top = later
    carried = early_top + later_total
    joint_top = jnp.maximum(carried, later_top)
    early_scale = jnp.exp(carried - joint_top)
    later_scale = jnp.exp(later_top - joint_top)
    memory = early_scale[:, None, None] * early_memory + later_scale[:, None, None] * later_memory
    normalizer = early_scale[:, None] * early_normalizer + later_scale[:, None] * later_normalizer
    return (early_total + later_total, memory, normalizer, joint_top)

def read_out(query_wide, keys_wide, values_wide, in_gate, log_cum, state):
    memory, normalizer, top_in = (state[1], state[2], state[3])
    length = query_wide.shape[0]
    lower_tri = jnp.tril(jnp.ones((length, length), dtype=bool))
    exponent = jnp.where(lower_tri[None], log_cum[:, :, None] - log_cum[:, None, :] + in_gate[:, None, :], -jnp.inf)
    before = log_cum + top_in[:, None]
    running = jnp.maximum(before, lax.optimization_barrier(jnp.max(exponent, axis=-1)))
    carry_scale = jnp.exp(before - running)
    scores = jnp.einsum('thd,shd->hts', query_wide, keys_wide, precision=highest) * QK_DIM ** (-0.5)
    weights = jnp.exp(exponent - running[:, :, None]) * scores
    rounded = lax.optimization_barrier(weights.astype(jnp.bfloat16)).astype(jnp.float32)
    numerator = carry_scale[:, :, None] * jnp.einsum('thd,hde->hte', query_wide, memory, precision=highest)
    numerator = numerator + jnp.einsum('hts,she->hte', rounded, values_wide, precision=highest)
    denominator = carry_scale * jnp.einsum('thd,hd->ht', query_wide, normalizer, precision=highest) + lax.optimization_barrier(jnp.sum(weights, axis=-1))
    return numerator / jnp.maximum(jnp.abs(denominator), jnp.exp(-running))[:, :, None]

def one_direction(query_wide, keys_wide, values_wide, in_gate, forget_pre):
    blocks = TOKENS // TOK_DEV
    head_count = in_gate.shape[0]
    log_keep = jax.nn.log_sigmoid(forget_pre)

    def cut_rows(array):
        return array.reshape((blocks, TOK_DEV) + array.shape[1:])

    def cut_gate(array):
        return jnp.moveaxis(array.reshape(head_count, blocks, TOK_DEV), 1, 0)
    initial = (jnp.zeros((head_count,), jnp.float32), jnp.zeros((head_count, QK_DIM, V_DIM), jnp.float32), jnp.zeros((head_count, QK_DIM), jnp.float32), jnp.full((head_count,), floor_log, jnp.float32))

    def advance(state, piece):
        query_block, keys_block, values_block, gate_block, keep_block = piece
        log_cum = jnp.cumsum(keep_block, axis=-1)
        result = read_out(query_block, keys_block, values_block, gate_block, log_cum, state)
        summary = summarize(keys_block * QK_DIM ** (-0.5), values_block, gate_block, log_cum)
        return (combine(state, summary), result)
    _, results = lax.scan(advance, initial, (cut_rows(query_wide), cut_rows(keys_wide), cut_rows(values_wide), cut_gate(in_gate), cut_gate(log_keep)))
    return jnp.moveaxis(results, 0, 1).reshape(head_count, TOKENS, V_DIM)

def smear(upper, taps):
    side = CONV // 2
    padded = jnp.pad(upper.astype(jnp.float32), ((side, CONV - 1 - side), (0, 0)))
    total = padded[0:TOKENS] * taps[0]
    for offset in range(1, CONV):
        total = total + padded[offset:offset + TOKENS] * taps[offset]
    return total

def reference(residual, query, keys, values, out_gate, input_gate, forget_gate, head_gain, w_out, norm_gain, w_up_gate, w_up_value, conv_gate, conv_value, w_down):
    query_wide = query.astype(jnp.float32).reshape(TOKENS, HEADS, QK_DIM)
    keys_wide = keys.astype(jnp.float32).reshape(TOKENS, HEADS, QK_DIM)
    values_wide = values.astype(jnp.float32).reshape(TOKENS, HEADS, V_DIM)
    forward = one_direction(query_wide, keys_wide, values_wide, input_gate[0], forget_gate[0])
    backward = one_direction(jnp.flip(query_wide, axis=0), jnp.flip(keys_wide, axis=0), jnp.flip(values_wide, axis=0), jnp.flip(input_gate[1], axis=-1), jnp.flip(forget_gate[1], axis=-1))
    both = forward + jnp.flip(backward, axis=1)
    scaled = both * lax.rsqrt(lax.optimization_barrier(jnp.mean(both * both, axis=-1, keepdims=True)) + epsilon)
    scaled = scaled * head_gain.reshape(HEADS, V_DIM)[:, None, :]
    side_by_side = jnp.transpose(scaled, (1, 0, 2)).reshape(TOKENS, V_WIDTH)
    gated = (side_by_side * jax.nn.sigmoid(out_gate.astype(jnp.float32))).astype(jnp.bfloat16)
    stream = (residual.astype(jnp.float32) + jnp.dot(gated, w_out, preferred_element_type=jnp.float32)).astype(jnp.bfloat16)
    stream_wide = stream.astype(jnp.float32)
    normed = stream_wide * lax.rsqrt(lax.optimization_barrier(jnp.mean(stream_wide * stream_wide, axis=-1, keepdims=True)) + epsilon)
    normed = (normed * norm_gain).astype(jnp.bfloat16)
    up_gate = jnp.dot(normed, w_up_gate, preferred_element_type=jnp.float32).astype(jnp.bfloat16)
    up_value = jnp.dot(normed, w_up_value, preferred_element_type=jnp.float32).astype(jnp.bfloat16)
    hidden = (jax.nn.silu(smear(up_gate, conv_gate)) * smear(up_value, conv_value)).astype(jnp.bfloat16)
    return (stream_wide + jnp.dot(hidden, w_down, preferred_element_type=jnp.float32)).astype(jnp.bfloat16)
```

```python
import jax
import jax.numpy as jnp
from jax import lax
from jax.sharding import PartitionSpec as P

QK_DIM = 128
V_DIM = 256
CONV = 3

epsilon = 1e-06
floor_log = -1e30
highest = lax.Precision.HIGHEST


def shift(value, axis, k):
    n = lax.axis_size(axis)
    return lax.ppermute(value, axis, [(i, (i + k) % n) for i in range(n)])


def flip_bit(value, axis, mask):
    n = lax.axis_size(axis)
    return lax.ppermute(value, axis, [(i, i ^ mask) for i in range(n)])


def move(value, axis, k):
    n = lax.axis_size(axis)
    return lax.ppermute(value, axis, [(i, i + k) for i in range(n) if 0 <= i + k < n])


def gather_flips(value, axis):
    n = lax.axis_size(axis)
    found = {0: value}
    bit = n >> 1
    while bit:
        for mask in list(found):
            found[mask | bit] = flip_bit(found[mask], axis, bit)
        bit >>= 1
    return found


def weight_parts(value):
    n, mine = lax.axis_size("sp"), lax.axis_index("sp")
    groups, here = lax.axis_size("grp"), lax.axis_index("grp")
    size = value.shape[0] // groups
    half = lax.dynamic_slice_in_dim(value, here * size, size, axis=0)
    order = []
    for k in range(1, n):
        back = (k + 1) // 2 if k % 2 else n - k // 2
        order.append(back)
    result = []
    for k in order:
        straight = shift(half, "sp", k)
        parts = [(here, straight)]
        for j in range(1, groups):
            parts.append(((here - j) % groups, shift(straight, "grp", j)))
        result.append(((mine - k) % n, parts))
    return result


def direction(query, keys, values, scores, gate, cum, total, lower, sign):
    growth = total - cum + gate
    largest = jnp.max(growth)
    weighting = jnp.exp(growth - largest)
    weighted = keys.astype(jnp.float32) * (weighting * QK_DIM ** (-0.5))[:, None]
    memory = jnp.einsum("sd,se->de", weighted, values.astype(jnp.float32), precision=highest)
    normalizer = jnp.sum(weighted, axis=0)
    small = jnp.zeros((8, V_DIM), jnp.float32)
    small = small.at[0, :QK_DIM].set(normalizer).at[1, :128].set(total).at[1, 128:].set(largest)
    packed = jnp.concatenate([memory, small], axis=0)

    n, mine = lax.axis_size("sp"), lax.axis_index("sp")
    exponents, pieces = [], []
    gone = jnp.float32(0.0)
    for k in range(1, n):
        piece = move(packed, "sp", sign * k)
        valid = (mine - k >= 0) if sign > 0 else (mine + k < n)
        exponents.append(jnp.where(valid, piece[QK_DIM + 1, 128] + gone, floor_log))
        gone = gone + piece[QK_DIM + 1, 0]
        pieces.append(piece)
    top_in = jnp.float32(floor_log)
    for a in exponents:
        top_in = jnp.maximum(top_in, a)
    state = sum(jnp.exp(a - top_in) * p[: QK_DIM + 1] for a, p in zip(exponents, pieces))
    memory_in, normalizer_in = state[:QK_DIM], state[QK_DIM, :QK_DIM]

    exponent = jnp.where(lower, cum[:, None] - cum[None, :] + gate[None, :], -jnp.inf)
    before = cum + top_in
    running = jnp.maximum(before, jnp.max(exponent, axis=-1))
    carry = jnp.exp(before - running)
    weights = jnp.exp(exponent - running[:, None]) * scores
    query_wide = query.astype(jnp.float32)
    numerator = carry[:, None] * jnp.dot(query_wide, memory_in, precision=highest)
    numerator = numerator + jnp.dot(
        weights.astype(jnp.bfloat16), values, preferred_element_type=jnp.float32
    )
    denominator = carry * jnp.sum(query_wide * normalizer_in[None, :], axis=-1)
    denominator = denominator + jnp.sum(weights, axis=-1)
    return numerator / jnp.maximum(jnp.abs(denominator), jnp.exp(-running))[:, None]


def heads(query, keys, values, out_gate, input_gate, forget_gate, head_gain):
    length = query.shape[0]
    rows = lax.broadcasted_iota(jnp.int32, (length, length), 0)
    columns = lax.broadcasted_iota(jnp.int32, (length, length), 1)
    log_keep = jax.nn.log_sigmoid(forget_gate)
    ahead_cum = lax.cumsum(log_keep[0], axis=1)
    behind_cum = lax.cumsum(log_keep[1], axis=1, reverse=True)
    gated = []
    for h in range(input_gate.shape[1]):
        q = query[:, h * QK_DIM : (h + 1) * QK_DIM]
        k = keys[:, h * QK_DIM : (h + 1) * QK_DIM]
        wide = slice(h * V_DIM, (h + 1) * V_DIM)
        v = values[:, wide]
        scores = jnp.einsum("td,sd->ts", q, k, preferred_element_type=jnp.float32)
        scores = scores * QK_DIM ** (-0.5)
        ahead = direction(
            q, k, v, scores, input_gate[0, h], ahead_cum[h], ahead_cum[h, -1], columns <= rows, 1
        )
        behind = direction(
            q, k, v, scores, input_gate[1, h], behind_cum[h], behind_cum[h, 0], columns >= rows, -1
        )
        both = ahead + behind
        scaled = both * lax.rsqrt(jnp.mean(both * both, axis=-1, keepdims=True) + epsilon)
        scaled = scaled * head_gain[wide][None, :]
        gated.append(
            (scaled * jax.nn.sigmoid(out_gate[:, wide].astype(jnp.float32))).astype(jnp.bfloat16)
        )
    return gated[0] if len(gated) == 1 else jnp.concatenate(gated, axis=1)


def local(
    residual,
    query,
    keys,
    values,
    out_gate,
    input_gate,
    forget_gate,
    head_gain,
    w_out,
    norm_gain,
    w_up_gate,
    w_up_value,
    conv_gate,
    conv_value,
    w_down,
):
    length = query.shape[0]
    tile = residual.shape[0]
    tp_mine, sp_mine = lax.axis_index("tp"), lax.axis_index("sp")
    few = lax.axis_size("sp") <= 8

    w_up = jnp.concatenate([w_up_gate, w_up_value], axis=1)
    if few:
        up_parts = weight_parts(w_up)
        down_parts = weight_parts(w_down)
    else:
        up_whole = lax.all_gather(w_up, "sp", axis=0, tiled=True)
        down_whole = lax.all_gather(w_down, "sp", axis=1, tiled=True)
    out_blocks = gather_flips(w_out, "tp")
    residual_blocks = gather_flips(residual, "tp")
    stream = jnp.zeros((length, residual.shape[1]), jnp.bfloat16)
    for mask, block in residual_blocks.items():
        stream = lax.dynamic_update_slice_in_dim(stream, block, (tp_mine ^ mask) * tile, axis=0)

    gated = heads(query, keys, values, out_gate, input_gate, forget_gate, head_gain)
    gated_blocks = gather_flips(gated, "tp")
    wide = stream.astype(jnp.float32)
    for mask, block in gated_blocks.items():
        wide = wide + jnp.dot(block, out_blocks[mask], preferred_element_type=jnp.float32)
    stream = wide.astype(jnp.bfloat16)
    wide = stream.astype(jnp.float32)
    normed = wide * lax.rsqrt(jnp.mean(wide * wide, axis=-1, keepdims=True) + epsilon)
    normed = (normed * norm_gain).astype(jnp.bfloat16)
    before = move(normed[length - 1 :], "sp", 1)
    after = move(normed[:1], "sp", -1)
    fill = jnp.zeros((14, normed.shape[1]), jnp.bfloat16)
    normed = jnp.concatenate([normed, before, after, fill], axis=0)

    depth = w_up.shape[0]
    if few:

        def term(start, rows):
            part = lax.dynamic_slice_in_dim(normed, start, rows.shape[0], axis=1)
            return jnp.dot(part, rows, preferred_element_type=jnp.float32)

        upper = term(sp_mine * depth, w_up)
        for source, parts in up_parts:
            for part, rows in parts:
                upper = upper + term(source * depth + part * rows.shape[0], rows)
    else:
        upper = jnp.dot(normed, up_whole, preferred_element_type=jnp.float32)
    upper = upper.astype(jnp.bfloat16)
    padded = jnp.concatenate([upper[length : length + 1], upper[:length], upper[length + 1 : length + 2]], axis=0)
    taps = jnp.concatenate([conv_gate, conv_value], axis=1)
    smeared = padded[0:length] * taps[0]
    for offset in range(1, CONV):
        smeared = smeared + padded[offset : offset + length] * taps[offset]
    width_ff = w_up_gate.shape[1]
    hidden = (jax.nn.silu(smeared[:, :width_ff]) * smeared[:, width_ff:]).astype(jnp.bfloat16)

    own = lax.dynamic_slice_in_dim(stream, tp_mine * tile, tile, axis=0).astype(jnp.float32)
    if few:
        blocks = [(sp_mine, jnp.dot(hidden, w_down, preferred_element_type=jnp.float32))]
        for source, parts in down_parts:
            terms = None
            for part, rows in parts:
                piece = lax.dynamic_slice_in_dim(hidden, part * rows.shape[0], rows.shape[0], axis=1)
                piece = jnp.dot(piece, rows, preferred_element_type=jnp.float32)
                terms = piece if terms is None else terms + piece
            blocks.append((source, terms))
        returned = jnp.zeros((tile, residual.shape[1]), jnp.float32)
        for source, terms in blocks:
            total = reduce_rows(terms, tile)
            returned = lax.dynamic_update_slice_in_dim(
                returned, total, source * total.shape[1], axis=1
            )
    else:
        returned = reduce_rows(jnp.dot(hidden, down_whole, preferred_element_type=jnp.float32), tile)
    return (own + returned).astype(jnp.bfloat16)


def reduce_rows(terms, tile):
    n, mine = lax.axis_size("tp"), lax.axis_index("tp")
    columns = terms.shape[1]
    terms = terms.reshape(n, tile, columns)
    bit = 1
    while bit < n:
        pairs = terms.reshape(terms.shape[0] // 2, 2, tile, columns)
        side = (mine // bit) % 2
        kept = lax.dynamic_index_in_dim(pairs, side, axis=1, keepdims=False)
        sent = lax.dynamic_index_in_dim(pairs, 1 - side, axis=1, keepdims=False)
        got = flip_bit(sent.astype(jnp.bfloat16), "tp", bit)
        terms = kept + got.astype(jnp.float32)
        bit *= 2
    return terms[0]


def solution(mesh):
    placed = (
        P(("grp", "sp", "tp"), None),
        P(("grp", "sp"), "tp"),
        P(("grp", "sp"), "tp"),
        P(("grp", "sp"), "tp"),
        P(("grp", "sp"), "tp"),
        P(None, "tp", ("grp", "sp")),
        P(None, "tp", ("grp", "sp")),
        P("tp"),
        P("tp", None),
        P(),
        P("sp", "tp"),
        P("sp", "tp"),
        P(None, "tp"),
        P(None, "tp"),
        P("tp", "sp"),
    )
    return jax.shard_map(
        local, mesh=mesh, in_specs=placed, out_specs=P(("grp", "sp", "tp"), None), check_vma=False
    )
```

```python
import jax
import jax.numpy as jnp
from jax import lax
from jax.experimental import pallas as pl
from jax.experimental.pallas import tpu as pltpu
from jax.sharding import PartitionSpec as P

QK_DIM = 128
V_DIM = 256
CONV = 3

epsilon = 1e-06
floor_log = -1e30
highest = lax.Precision.HIGHEST


def shift(value, axis, k):
    n = lax.axis_size(axis)
    return lax.ppermute(value, axis, [(i, (i + k) % n) for i in range(n)])


def flip_bit(value, axis, mask):
    n = lax.axis_size(axis)
    return lax.ppermute(value, axis, [(i, i ^ mask) for i in range(n)])


def move(value, axis, k):
    n = lax.axis_size(axis)
    return lax.ppermute(value, axis, [(i, i + k) for i in range(n) if 0 <= i + k < n])


def gather_flips(value, axis):
    n = lax.axis_size(axis)
    found = {0: value}
    bit = n >> 1
    while bit:
        for mask in list(found):
            found[mask | bit] = flip_bit(found[mask], axis, bit)
        bit >>= 1
    return found


def weight_parts(value):
    n, mine = lax.axis_size("sp"), lax.axis_index("sp")
    groups, here = lax.axis_size("grp"), lax.axis_index("grp")
    size = value.shape[0] // groups
    half = lax.dynamic_slice_in_dim(value, here * size, size, axis=0)
    order = []
    for k in range(1, n):
        back = (k + 1) // 2 if k % 2 else n - k // 2
        order.append(back)
    result = []
    for k in order:
        straight = shift(half, "sp", k)
        parts = [(here, straight)]
        for j in range(1, groups):
            parts.append(((here - j) % groups, shift(straight, "grp", j)))
        result.append(((mine - k) % n, parts))
    return result


def direction(query, keys, values, scores, gate, cum, total, lower, sign):
    growth = total - cum + gate
    largest = jnp.max(growth)
    weighting = jnp.exp(growth - largest)
    weighted = keys.astype(jnp.float32) * (weighting * QK_DIM ** (-0.5))[:, None]
    memory = jnp.einsum("sd,se->de", weighted, values.astype(jnp.float32), precision=highest)
    normalizer = jnp.sum(weighted, axis=0)
    small = jnp.zeros((8, V_DIM), jnp.float32)
    small = small.at[0, :QK_DIM].set(normalizer).at[1, :128].set(total).at[1, 128:].set(largest)
    packed = jnp.concatenate([memory, small], axis=0)

    n, mine = lax.axis_size("sp"), lax.axis_index("sp")
    exponents, pieces = [], []
    gone = jnp.float32(0.0)
    for k in range(1, n):
        piece = move(packed, "sp", sign * k)
        valid = (mine - k >= 0) if sign > 0 else (mine + k < n)
        exponents.append(jnp.where(valid, piece[QK_DIM + 1, 128] + gone, floor_log))
        gone = gone + piece[QK_DIM + 1, 0]
        pieces.append(piece)
    top_in = jnp.float32(floor_log)
    for a in exponents:
        top_in = jnp.maximum(top_in, a)
    state = sum(jnp.exp(a - top_in) * p[: QK_DIM + 1] for a, p in zip(exponents, pieces))
    memory_in, normalizer_in = state[:QK_DIM], state[QK_DIM, :QK_DIM]

    exponent = jnp.where(lower, cum[:, None] - cum[None, :] + gate[None, :], -jnp.inf)
    before = cum + top_in
    running = jnp.maximum(before, jnp.max(exponent, axis=-1))
    carry = jnp.exp(before - running)
    weights = jnp.exp(exponent - running[:, None]) * scores
    query_wide = query.astype(jnp.float32)
    numerator = carry[:, None] * jnp.dot(query_wide, memory_in, precision=highest)
    numerator = numerator + jnp.dot(
        weights.astype(jnp.bfloat16), values, preferred_element_type=jnp.float32
    )
    denominator = carry * jnp.sum(query_wide * normalizer_in[None, :], axis=-1)
    denominator = denominator + jnp.sum(weights, axis=-1)
    return numerator / jnp.maximum(jnp.abs(denominator), jnp.exp(-running))[:, None]


def heads(query, keys, values, out_gate, input_gate, forget_gate, head_gain):
    length = query.shape[0]
    rows = lax.broadcasted_iota(jnp.int32, (length, length), 0)
    columns = lax.broadcasted_iota(jnp.int32, (length, length), 1)
    log_keep = jax.nn.log_sigmoid(forget_gate)
    ahead_cum = lax.cumsum(log_keep[0], axis=1)
    behind_cum = lax.cumsum(log_keep[1], axis=1, reverse=True)
    gated = []
    for h in range(input_gate.shape[1]):
        q = query[:, h * QK_DIM : (h + 1) * QK_DIM]
        k = keys[:, h * QK_DIM : (h + 1) * QK_DIM]
        wide = slice(h * V_DIM, (h + 1) * V_DIM)
        v = values[:, wide]
        scores = jnp.einsum("td,sd->ts", q, k, preferred_element_type=jnp.float32)
        scores = scores * QK_DIM ** (-0.5)
        ahead = direction(
            q, k, v, scores, input_gate[0, h], ahead_cum[h], ahead_cum[h, -1], columns <= rows, 1
        )
        behind = direction(
            q, k, v, scores, input_gate[1, h], behind_cum[h], behind_cum[h, 0], columns >= rows, -1
        )
        both = ahead + behind
        scaled = both * lax.rsqrt(jnp.mean(both * both, axis=-1, keepdims=True) + epsilon)
        scaled = scaled * head_gain[wide][None, :]
        gated.append(
            (scaled * jax.nn.sigmoid(out_gate[:, wide].astype(jnp.float32))).astype(jnp.bfloat16)
        )
    return gated[0] if len(gated) == 1 else jnp.concatenate(gated, axis=1)


def local(
    residual,
    query,
    keys,
    values,
    out_gate,
    input_gate,
    forget_gate,
    head_gain,
    w_out,
    norm_gain,
    w_up_gate,
    w_up_value,
    conv_gate,
    conv_value,
    w_down,
):
    length = query.shape[0]
    tile = residual.shape[0]
    tp_mine, sp_mine = lax.axis_index("tp"), lax.axis_index("sp")
    few = lax.axis_size("sp") <= 8

    w_up = jnp.concatenate([w_up_gate, w_up_value], axis=1)
    if few:
        up_parts = weight_parts(w_up)
        down_parts = weight_parts(w_down)
    else:
        up_whole = lax.all_gather(w_up, "sp", axis=0, tiled=True)
        down_whole = lax.all_gather(w_down, "sp", axis=1, tiled=True)
    out_blocks = gather_flips(w_out, "tp")
    residual_blocks = gather_flips(residual, "tp")
    stream = jnp.zeros((length, residual.shape[1]), jnp.bfloat16)
    for mask, block in residual_blocks.items():
        stream = lax.dynamic_update_slice_in_dim(stream, block, (tp_mine ^ mask) * tile, axis=0)

    gated = heads(query, keys, values, out_gate, input_gate, forget_gate, head_gain)
    gated_blocks = gather_flips(gated, "tp")
    wide = stream.astype(jnp.float32)
    for mask, block in gated_blocks.items():
        wide = wide + jnp.dot(block, out_blocks[mask], preferred_element_type=jnp.float32)
    stream = wide.astype(jnp.bfloat16)
    wide = stream.astype(jnp.float32)
    normed = wide * lax.rsqrt(jnp.mean(wide * wide, axis=-1, keepdims=True) + epsilon)
    normed = (normed * norm_gain).astype(jnp.bfloat16)
    before = move(normed[length - 1 :], "sp", 1)
    after = move(normed[:1], "sp", -1)
    fill = jnp.zeros((14, normed.shape[1]), jnp.bfloat16)
    normed = jnp.concatenate([normed, before, after, fill], axis=0)

    depth = w_up.shape[0]
    if few:

        def term(start, rows):
            part = lax.dynamic_slice_in_dim(normed, start, rows.shape[0], axis=1)
            return jnp.dot(part, rows, preferred_element_type=jnp.float32)

        upper = term(sp_mine * depth, w_up)
        for source, parts in up_parts:
            for part, rows in parts:
                upper = upper + term(source * depth + part * rows.shape[0], rows)
    else:
        upper = jnp.dot(normed, up_whole, preferred_element_type=jnp.float32)
    upper = upper.astype(jnp.bfloat16)
    padded = jnp.concatenate([upper[length : length + 1], upper[:length], upper[length + 1 : length + 2]], axis=0)
    taps = jnp.concatenate([conv_gate, conv_value], axis=1)
    smeared = padded[0:length] * taps[0]
    for offset in range(1, CONV):
        smeared = smeared + padded[offset : offset + length] * taps[offset]
    width_ff = w_up_gate.shape[1]
    hidden = (jax.nn.silu(smeared[:, :width_ff]) * smeared[:, width_ff:]).astype(jnp.bfloat16)

    own = lax.dynamic_slice_in_dim(stream, tp_mine * tile, tile, axis=0).astype(jnp.float32)
    if few:
        blocks = [(sp_mine, jnp.dot(hidden, w_down, preferred_element_type=jnp.float32))]
        for source, parts in down_parts:
            terms = None
            for part, rows in parts:
                piece = lax.dynamic_slice_in_dim(hidden, part * rows.shape[0], rows.shape[0], axis=1)
                piece = jnp.dot(piece, rows, preferred_element_type=jnp.float32)
                terms = piece if terms is None else terms + piece
            blocks.append((source, terms))
        returned = jnp.zeros((tile, residual.shape[1]), jnp.float32)
        for source, terms in blocks:
            total = reduce_rows(terms, tile)
            returned = lax.dynamic_update_slice_in_dim(
                returned, total, source * total.shape[1], axis=1
            )
    else:
        returned = reduce_rows(jnp.dot(hidden, down_whole, preferred_element_type=jnp.float32), tile)
    return (own + returned).astype(jnp.bfloat16)


def reduce_rows(terms, tile):
    n, mine = lax.axis_size("tp"), lax.axis_index("tp")
    columns = terms.shape[1]
    terms = terms.reshape(n, tile, columns)
    bit = 1
    while bit < n:
        pairs = terms.reshape(terms.shape[0] // 2, 2, tile, columns)
        side = (mine // bit) % 2
        kept = lax.dynamic_index_in_dim(pairs, side, axis=1, keepdims=False)
        sent = lax.dynamic_index_in_dim(pairs, 1 - side, axis=1, keepdims=False)
        got = flip_bit(sent.astype(jnp.bfloat16), "tp", bit)
        terms = kept + got.astype(jnp.float32)
        bit *= 2
    return terms[0]


LANE = 128


def cut_kernel(quarter, index, gate, value, down, up_out, down_out):
    limit = gate.shape[1]
    for i in range(2):
        for share in range(4):
            start = share * quarter
            size = min(quarter, limit - start)

            @pl.when(index[i] == share)
            def _():
                if size < quarter:
                    up_out[i] = jnp.zeros(up_out.shape[1:], up_out.dtype)
                    down_out[i] = jnp.zeros(down_out.shape[1:], down_out.dtype)
                up_out[i, :, :size] = gate[:, start : start + size]
                up_out[i, :, quarter : quarter + size] = value[:, start : start + size]
                down_out[i, :size] = down[start : start + size]


def cut_weights(index, w_up_gate, w_up_value, w_down, quarter):
    depth, out = w_up_gate.shape[0], w_down.shape[1]
    vmem = pl.BlockSpec(memory_space=pltpu.VMEM)
    return pl.pallas_call(
        lambda *refs: cut_kernel(quarter, *refs),
        out_shape=(
            jax.ShapeDtypeStruct((2, depth, 2 * quarter), w_up_gate.dtype),
            jax.ShapeDtypeStruct((2, quarter, out), w_down.dtype),
        ),
        in_specs=[pl.BlockSpec(memory_space=pltpu.SMEM), vmem, vmem, vmem],
        out_specs=[vmem, vmem],
        compiler_params=pltpu.CompilerParams(vmem_limit_bytes=24 * 2**20),
    )(index, w_up_gate, w_up_value, w_down)


def gather_pair(blocks, order):
    position = {"grp": 0, "sp": 1, "tp": 2}
    for axis, bit in order:
        keys = sorted(blocks)
        sent = jnp.concatenate([blocks[k] for k in keys], axis=0) if len(keys) > 1 else blocks[keys[0]]
        got = flip_bit(sent, axis, bit)
        size = got.shape[0] // len(keys)
        for i, k in enumerate(keys):
            other = list(k)
            other[position[axis]] |= bit
            blocks[tuple(other)] = got[i * size : (i + 1) * size]
    return blocks


def reduce_pair(terms, order):
    mine = lax.axis_index("tp")
    for axis, bit in order:
        if axis == "grp":
            kept, sent = terms[0:1], terms[1:2]
        elif axis == "sp":
            kept, sent = terms[:, 0:1], terms[:, 1:2]
        else:
            where = 3 if bit == 1 else 2
            side = (mine // bit) % 2
            kept = lax.dynamic_slice_in_dim(terms, side, 1, axis=where)
            sent = lax.dynamic_slice_in_dim(terms, 1 - side, 1, axis=where)
        got = flip_bit(sent.astype(jnp.bfloat16), axis, bit)
        terms = kept.astype(jnp.float32) + got.astype(jnp.float32)
    return terms.reshape(terms.shape[-2:])


def shared(
    residual, query, keys, values, out_gate, input_gate, forget_gate, head_gain,
    w_out, norm_gain, w_up_gate, w_up_value, conv_gate, conv_value, w_down,
):
    length, tile, model = query.shape[0], residual.shape[0], residual.shape[1]
    tp_mine, sp_mine, g_mine = lax.axis_index("tp"), lax.axis_index("sp"), lax.axis_index("grp")
    parity = sp_mine % 2
    width_ff = w_up_gate.shape[1]
    quarter = -(-width_ff // (4 * LANE)) * LANE
    share = g_mine * 2 + parity
    index = jnp.stack([share, g_mine * 2 + 1 - parity]).astype(jnp.int32)
    up_cut, down_cut = cut_weights(index, w_up_gate, w_up_value, w_down, quarter)
    up_of, down_of = {0: up_cut[0]}, {0: down_cut[0]}
    for mask in (1, 2, 3):
        up_of[mask] = flip_bit(up_cut[mask % 2], "sp", mask)
    for mask in (1, 2, 3):
        down_of[mask] = flip_bit(down_cut[mask % 2], "sp", mask)
    out_blocks = gather_flips(w_out, "tp")
    tp_bits = [2**i for i in range(lax.axis_size("tp").bit_length() - 1)]
    far = [("tp", bit) for bit in tp_bits if bit > 1]
    near = [("tp", 1)]
    residual_blocks = gather_pair(
        {(0, 0, 0): residual}, [("sp", 1), ("grp", 1)] + far + near
    )
    streams = []
    for g in range(2):
        for z in range(2):
            block = jnp.zeros((length, model), jnp.bfloat16)
            for mask in range(lax.axis_size("tp")):
                block = lax.dynamic_update_slice_in_dim(
                    block, residual_blocks[g, z, mask], (tp_mine ^ mask) * tile, axis=0
                )
            streams.append(block)

    gated = heads(query, keys, values, out_gate, input_gate, forget_gate, head_gain)
    half = length // 2
    orders = (
        [("sp", 1), ("grp", 1)] + far + near,
        far + [("grp", 1), ("sp", 1)] + near,
    )
    found = [
        gather_pair({(0, 0, 0): gated[c * half : (c + 1) * half]}, order)
        for c, order in enumerate(orders)
    ]
    wide = jnp.concatenate(streams, axis=0).astype(jnp.float32)
    for mask in range(lax.axis_size("tp")):
        rows = jnp.concatenate(
            [found[c][g, z, mask] for g in range(2) for z in range(2) for c in range(2)], axis=0
        )
        wide = wide + jnp.dot(rows, out_blocks[mask], preferred_element_type=jnp.float32)
    stream = wide.astype(jnp.bfloat16)
    own = lax.dynamic_slice_in_dim(stream, tp_mine * tile, tile, axis=0).astype(jnp.float32)
    wide = stream.astype(jnp.float32)
    normed = wide * lax.rsqrt(jnp.mean(wide * wide, axis=-1, keepdims=True) + epsilon)
    normed = (normed * norm_gain).astype(jnp.bfloat16)
    first = [normed[2 * g * length : 2 * g * length + 1] for g in range(2)]
    first_other = [normed[(2 * g + 1) * length : (2 * g + 1) * length + 1] for g in range(2)]
    last = [normed[(2 * g + 1) * length - 1 : (2 * g + 1) * length] for g in range(2)]
    last_other = [normed[(2 * g + 2) * length - 1 : (2 * g + 2) * length] for g in range(2)]
    low = parity == 0
    first = jnp.where(low, jnp.concatenate(first, axis=0), jnp.concatenate(first_other, axis=0))
    last = jnp.where(low, jnp.concatenate(last_other, axis=0), jnp.concatenate(last, axis=0))
    before = move(last, "sp", 2)
    after = move(first, "sp", -2)
    fill = jnp.zeros((12, model), jnp.bfloat16)
    edges = jnp.concatenate([before, after, fill], axis=0)

    depth = w_up_gate.shape[0]
    upper = edge = None
    for mask in (0, 1, 2, 3):
        start = (sp_mine ^ mask) * depth
        part = lax.dynamic_slice_in_dim(normed, start, depth, axis=1)
        side = lax.dynamic_slice_in_dim(edges, start, depth, axis=1)
        term = jnp.dot(part, up_of[mask], preferred_element_type=jnp.float32)
        brim = jnp.dot(side, up_of[mask], preferred_element_type=jnp.float32)
        upper = term if upper is None else upper + term
        edge = brim if edge is None else edge + brim
    upper = upper.astype(jnp.bfloat16).reshape(2, 2, length, 2 * quarter)
    edge = edge.astype(jnp.bfloat16)
    spare = 4 * quarter - width_ff

    def taps_of(taps):
        return lax.dynamic_slice_in_dim(jnp.pad(taps, ((0, 0), (0, spare))), share * quarter, quarter, axis=1)

    taps = jnp.concatenate([taps_of(conv_gate), taps_of(conv_value)], axis=1)
    hidden = []
    for g in range(2):
        for z in range(2):
            here, other = upper[g, z], upper[g, 1 - z]
            above = low if z == 0 else jnp.logical_not(low)
            previous = jnp.where(above, edge[g : g + 1], other[length - 1 :])
            following = jnp.where(above, other[:1], edge[2 + g : 3 + g])
            padded = jnp.concatenate([previous, here, following], axis=0)
            smeared = padded[0:length] * taps[0]
            for offset in range(1, CONV):
                smeared = smeared + padded[offset : offset + length] * taps[offset]
            gate, value = smeared[:, :quarter], smeared[:, quarter:]
            hidden.append((jax.nn.silu(gate) * value).astype(jnp.bfloat16))
    hidden = jnp.concatenate(hidden, axis=0)

    rounds = (
        near + [("grp", 1), ("sp", 1)] + far,
        near + [("sp", 1)] + far + [("grp", 1)],
        near + far + [("grp", 1), ("sp", 1)],
        near + [("grp", 1)] + far + [("sp", 1)],
    )
    returned = jnp.zeros((tile, model), jnp.float32)
    for mask in (0, 1, 2, 3):
        block = jnp.where(low, down_of[mask], down_of[mask ^ 1])
        terms = jnp.dot(hidden, block, preferred_element_type=jnp.float32)
        terms = terms.reshape(2, 2, lax.axis_size("tp") // 2, 2, tile, terms.shape[1])
        total = reduce_pair(terms, rounds[mask])
        returned = lax.dynamic_update_slice_in_dim(
            returned, total, ((sp_mine - parity) ^ mask) * total.shape[1], axis=1
        )
    return (own + returned).astype(jnp.bfloat16)


def solution(mesh):
    placed = (
        P(("grp", "sp", "tp"), None),
        P(("grp", "sp"), "tp"),
        P(("grp", "sp"), "tp"),
        P(("grp", "sp"), "tp"),
        P(("grp", "sp"), "tp"),
        P(None, "tp", ("grp", "sp")),
        P(None, "tp", ("grp", "sp")),
        P("tp"),
        P("tp", None),
        P(),
        P("sp", "tp"),
        P("sp", "tp"),
        P(None, "tp"),
        P(None, "tp"),
        P("tp", "sp"),
    )
    shared_form = (mesh.shape["grp"], mesh.shape["sp"], mesh.shape["tp"]) == (2, 4, 4)
    return jax.shard_map(
        shared if shared_form else local, mesh=mesh, in_specs=placed, out_specs=P(("grp", "sp", "tp"), None), check_vma=False
    )
```
